32 devices in a mesh: dp: 4 (over y, x), kv: 4 (over z), tp: 2 (over core).
Axes of the slice: x: 2, y: 2, z: 4, core: 2. Of those that a mesh axis runs over, the one named last changes fastest.
Arguments:
- tokens: bfloat16 [128, 2048], P('dp', ('kv', 'tp')), may hold values from -60 to 60
- first_norm_gain: float32 [2048], replicated, may hold values from 0.1 to 1.9
- first_gate_weight: bfloat16 [2048, 5632], P(None, ('kv', 'tp')), may hold values from -0.125 to 0.125
- first_up_weight: bfloat16 [2048, 5632], P(None, ('kv', 'tp')), may hold values from -0.125 to 0.125
- first_down_weight: bfloat16 [5632, 2048], P(('kv', 'tp')), may hold values from -0.109375 to 0.109375
- mixer_norm_gain: float32 [2048], replicated, may hold values from 0.1 to 1.9
- query_weight: bfloat16 [2048, 1024], P('kv', 'tp'), may hold values from -0.125 to 0.125
- key_weight: bfloat16 [2048, 1024], P('kv', 'tp'), may hold values from -0.125 to 0.125
- value_weight: bfloat16 [2048, 1024], P('kv', 'tp'), may hold values from -0.125 to 0.125
- output_gate_weight: bfloat16 [2048, 1024], P('kv', 'tp'), may hold values from -0.125 to 0.125
- strength_weight: bfloat16 [2048, 8], replicated, may hold values from -0.125 to 0.125
- decay_weight: bfloat16 [2048, 8], replicated, may hold values from -0.125 to 0.125
- head_decay_log: float32 [8], replicated, may hold values from 0 to 2.77
- decay_input_bias: float32 [8], replicated, may hold values from -4 to 0
- decay_extra_log: float32 [128, 8], P(('dp', 'kv'), 'tp'), may hold values from -0.7 to 0
- head_norm_gain: float32 [128], replicated, may hold values from 0.1 to 1.9
- state: float32 [128, 8, 128, 128], P(('dp', 'kv'), 'tp'), may hold values from -0.6 to 0.6
- mixer_output_weight: bfloat16 [1024, 2048], P('tp', 'kv'), may hold values from -0.1875 to 0.1875
- second_norm_gain: float32 [2048], replicated, may hold values from 0.1 to 1.9
- second_gate_weight: bfloat16 [2048, 5632], P(None, ('kv', 'tp')), may hold values from -0.125 to 0.125
- second_up_weight: bfloat16 [2048, 5632], P(None, ('kv', 'tp')), may hold values from -0.125 to 0.125
- second_down_weight: bfloat16 [5632, 2048], P(('kv', 'tp')), may hold values from -0.109375 to 0.109375
Outputs:
- layer_out: bfloat16 [128, 2048], P('dp', ('kv', 'tp'))
- new_state: float32 [128, 8, 128, 128], P(('dp', 'kv'), 'tp')
The draws below stay inside these ranges and needn't reach their ends.
All inputs are finite; a program needn't handle non-finite values.
Results may differ from the reference program's by a relative error of at most 0.014.
Values may be sent and summed in bfloat16 or wider, within the bound.
No kernel may reach another device: no remote copies, remote signals or barrier semaphores. Data moves between devices by JAX's collectives and lax.ppermute only.
A program may use at most 64 MiB of HBM per device.

```python
import jax
import jax.numpy as jnp
from jax import lax

D = 2048
FF = 5632
MIXER_HEADS = 8
HEAD_DIM = 128
SEQUENCE_COUNT = 128
N_TP = 2


def draw_tokens(key, part):
    base_key = jax.random.fold_in(key, 11)
    jitter_key = jax.random.fold_in(key, 12)
    rows_key = jax.random.fold_in(key, 13)
    column_pos = jnp.arange(D, dtype=jnp.float32) / D
    rising = 0.45 * jnp.exp(jnp.log(5.0) * column_pos)
    jitter = jnp.exp(jax.random.uniform(jitter_key, (D,), jnp.float32, -0.5, 0.5))
    row_scales = jnp.exp(jax.random.uniform(rows_key, (SEQUENCE_COUNT, 1), jnp.float32, -1.15, 1.15))
    base = jnp.clip(jax.random.normal(base_key, (SEQUENCE_COUNT, D), jnp.float32), -4.0, 4.0)
    return (base * rising * jitter * row_scales).astype(jnp.bfloat16)


def strengthened(drawn, rng, source, target, shards_of, factor):
    owner, partner = [(jnp.arange(drawn.shape[position]) // (drawn.shape[position] // shards_of)).reshape([-1 if axis == position else 1 for axis in range(drawn.ndim)]) for position in (source, target)]
    chosen = jax.random.permutation(rng, shards_of)[partner]
    strong = (owner == chosen) | (owner == (partner + shards_of // 2) % shards_of)
    return jnp.where(strong, factor * drawn, drawn)


def level_of(own_key, shape, split, low, high):
    def one(axis_at, blocks):
        draws = jax.random.uniform(jax.random.fold_in(jax.random.fold_in(own_key, 6), axis_at), (blocks,), jnp.float32, low / len(split), high / len(split))
        return jnp.repeat(jnp.exp(draws), shape[axis_at] // blocks).reshape((-1,) + (1,) * (len(shape) - axis_at - 1))

    gain = one(*split[0])
    for cut in split[1:]:
        gain = gain * one(*cut)
    return gain


def noise(own_key, dims, width, most, shards=(), held_as=jnp.bfloat16):
    level = level_of(own_key, dims, shards, -0.22, 0.18) if shards else 1.0
    array = jax.random.normal(own_key, dims, jnp.float32) * width * level
    return jnp.minimum(jnp.maximum(array, -most), most).astype(held_as)


def noise_with(rng, shape, spread, limit, cuts, heavy, held_as=jnp.bfloat16):
    array = spread * jax.random.normal(rng, shape, jnp.float32)
    if cuts:
        array = array * level_of(rng, shape, cuts, -0.22, 0.18)
    return jnp.clip(strengthened(array, jax.random.fold_in(rng, 3), *heavy), -limit, limit).astype(held_as)


def setup_inputs(seed: int = 0) -> dict:
    splits = jax.random.split(jax.random.key(seed), 23)
    return {
        "tokens": draw_tokens(jax.random.fold_in(splits[22], 71), 0),
        "first_norm_gain": jnp.clip(1.0 + 0.18 * jax.random.normal(splits[1], (D,), jnp.float32), 0.1, 1.9),
        "first_gate_weight": noise(splits[2], (D, FF), D ** -0.5, 0.125, ((1, 8),)),
        "first_up_weight": noise(splits[3], (D, FF), D ** -0.5, 0.125, ((1, 8),)),
        "first_down_weight": noise_with(splits[4], (FF, D), FF ** -0.5, 0.109375, ((0, 8),), (0, 1, 8, 2.0)),
        "mixer_norm_gain": jnp.clip(1.0 + 0.18 * jax.random.normal(splits[5], (D,), jnp.float32), 0.1, 1.9),
        "query_weight": noise(splits[6], (D, MIXER_HEADS * HEAD_DIM), D ** -0.5, 0.125, ((0, 4), (1, 2))),
        "key_weight": noise(splits[7], (D, MIXER_HEADS * HEAD_DIM), D ** -0.5, 0.125, ((0, 4), (1, 2))),
        "value_weight": noise(splits[8], (D, MIXER_HEADS * HEAD_DIM), D ** -0.5, 0.125, ((0, 4), (1, 2))),
        "output_gate_weight": noise(splits[9], (D, MIXER_HEADS * HEAD_DIM), D ** -0.5, 0.125, ((0, 4), (1, 2))),
        "strength_weight": noise(splits[10], (D, MIXER_HEADS), D ** -0.5, 0.125),
        "decay_weight": noise(splits[11], (D, MIXER_HEADS), D ** -0.5, 0.125),
        "head_decay_log": jnp.clip(jax.random.uniform(splits[12], (MIXER_HEADS,), jnp.float32, 0.0, 2.77), 0.0, 2.77),
        "decay_input_bias": jnp.clip(jax.random.uniform(splits[13], (MIXER_HEADS,), jnp.float32, -4.0, 0.0), -4.0, 0.0),
        "decay_extra_log": jnp.clip(-0.7 + 0.7 * jax.random.uniform(splits[14], (SEQUENCE_COUNT, MIXER_HEADS), jnp.float32) ** level_of(splits[14], (SEQUENCE_COUNT, MIXER_HEADS), ((0, 16), (1, 2)), -0.2, 0.2), -0.7, 0.0),
        "head_norm_gain": jnp.clip(1.0 + 0.18 * jax.random.normal(splits[15], (HEAD_DIM,), jnp.float32), 0.1, 1.9),
        "state": noise(splits[16], (SEQUENCE_COUNT, MIXER_HEADS, HEAD_DIM, HEAD_DIM), 0.1, 0.6, ((0, 16), (1, 2)), jnp.float32),
        "mixer_output_weight": noise(splits[17], (MIXER_HEADS * HEAD_DIM, D), (MIXER_HEADS * HEAD_DIM) ** -0.5, 0.1875, ((0, 2), (1, 4))),
        "second_norm_gain": jnp.clip(1.0 + 0.18 * jax.random.normal(splits[18], (D,), jnp.float32), 0.1, 1.9),
        "second_gate_weight": noise(splits[19], (D, FF), D ** -0.5, 0.125, ((1, 8),)),
        "second_up_weight": noise(splits[20], (D, FF), D ** -0.5, 0.125, ((1, 8),)),
        "second_down_weight": noise_with(splits[21], (FF, D), FF ** -0.5, 0.109375, ((0, 8),), (0, 1, 8, 2.0)),
    }


EPS = 1e-06

def row_scale(values):
    return lax.rsqrt(lax.optimization_barrier(jnp.mean(values * values, axis=-1, keepdims=True)) + EPS)

def unit_rows(values):
    return values * lax.rsqrt(lax.optimization_barrier(jnp.sum(values * values, axis=-1, keepdims=True)) + EPS)

def half_block(row_data, gain_vec, w_gate, w_up, w_down):
    rows32 = row_data.astype(jnp.float32)
    normed = (rows32 * row_scale(rows32) * gain_vec).astype(jnp.bfloat16)
    gate_pre = jnp.dot(normed, w_gate, preferred_element_type=jnp.float32)
    upward = jnp.dot(normed, w_up, preferred_element_type=jnp.float32)
    hidden = (jax.nn.silu(gate_pre) * upward).astype(jnp.bfloat16)
    return jnp.dot(hidden, w_down, preferred_element_type=jnp.float32)

def delta_step(query_vec, key_vec, value_vec, gate_vals, beta_gate, head_decay_rate, state, head_norm_gain):
    recalled = jnp.einsum('shd,shde->she', key_vec, state, precision=lax.Precision.HIGHEST)
    correction = beta_gate[..., None] * (value_vec - head_decay_rate[..., None] * recalled)
    new_state = head_decay_rate[..., None, None] * state + key_vec[..., :, None] * correction[..., None, :]
    read_out = jnp.einsum('shd,shde->she', query_vec, new_state, precision=lax.Precision.HIGHEST)
    normed = read_out * row_scale(read_out) * head_norm_gain
    return (normed * jax.nn.silu(gate_vals), new_state)

def reference(tokens, first_norm_gain, first_gate_weight, first_up_weight, first_down_weight, mixer_norm_gain, query_weight, key_weight, value_weight, output_gate_weight, strength_weight, decay_weight, head_decay_log, decay_input_bias, decay_extra_log, head_norm_gain, state, mixer_output_weight, second_norm_gain, second_gate_weight, second_up_weight, second_down_weight):
    batch_rows = tokens.shape[0]
    first_rows = (tokens.astype(jnp.float32) + 0.5 * half_block(tokens, first_norm_gain, first_gate_weight, first_up_weight, first_down_weight)).astype(jnp.bfloat16)
    first32 = first_rows.astype(jnp.float32)
    row_factor = row_scale(first32)
    scaled_rows = (first32 * mixer_norm_gain).astype(jnp.bfloat16)

    def apply_projection(weight):
        return row_factor * jnp.dot(scaled_rows, weight, preferred_element_type=jnp.float32)

    def split_heads(values):
        return values.reshape(batch_rows, MIXER_HEADS, HEAD_DIM)
    query_vec = unit_rows(jax.nn.silu(split_heads(apply_projection(query_weight)))) * HEAD_DIM ** (-0.5)
    key_vec = unit_rows(jax.nn.silu(split_heads(apply_projection(key_weight))))
    value_vec = jax.nn.silu(split_heads(apply_projection(value_weight)))
    gate_vals = split_heads(apply_projection(output_gate_weight))
    beta_gate = jax.nn.sigmoid(apply_projection(strength_weight))
    head_decay_rate = jnp.exp(decay_extra_log - jnp.exp(head_decay_log) * jax.nn.softplus(apply_projection(decay_weight) + decay_input_bias))
    heads_f32, new_state = delta_step(query_vec, key_vec, value_vec, gate_vals, beta_gate, head_decay_rate, state, head_norm_gain)
    heads_out = heads_f32.reshape(batch_rows, N_TP, MIXER_HEADS * HEAD_DIM // N_TP).astype(jnp.bfloat16)
    w_parts = mixer_output_weight.reshape(N_TP, MIXER_HEADS * HEAD_DIM // N_TP, D)
    mixer_sum = jnp.zeros((batch_rows, D), jnp.float32)
    for tp_part in range(N_TP):
        partial_value = jnp.dot(heads_out[:, tp_part], w_parts[tp_part], preferred_element_type=jnp.float32).astype(jnp.bfloat16)
        partial_value = lax.optimization_barrier(partial_value)
        mixer_sum = mixer_sum + partial_value.astype(jnp.float32)
    second_rows = (first32 + mixer_sum).astype(jnp.bfloat16)
    layer_out = (second_rows.astype(jnp.float32) + 0.5 * half_block(second_rows, second_norm_gain, second_gate_weight, second_up_weight, second_down_weight)).astype(jnp.bfloat16)
    return (layer_out, new_state)
```

```python
import jax
import jax.numpy as jnp
from jax import lax
from jax.sharding import PartitionSpec as P

EPS = 1e-06


def row_scale(values):
    return lax.rsqrt(jnp.mean(values * values, axis=-1, keepdims=True) + EPS)


def unit_rows(values):
    return values * lax.rsqrt(jnp.sum(values * values, axis=-1, keepdims=True) + EPS)


def swaps(axis, distance):
    return [(i, i ^ distance) for i in range(lax.axis_size(axis))]


def by_distance(blocks, own):
    blocks = list(blocks)
    bit = 1
    while bit < len(blocks):
        flip = (own & bit) != 0
        blocks = [jnp.where(flip, blocks[s ^ bit], blocks[s]) for s in range(len(blocks))]
        bit *= 2
    return blocks


def exchange(blocks, axis):
    return [blocks[0]] + [
        lax.ppermute(blocks[s], axis, swaps(axis, s)) for s in range(1, len(blocks))
    ]


def gathered(block, axis, own):
    return by_distance(exchange([block] * lax.axis_size(axis), axis), own)


def add_up(blocks):
    total = blocks[0].astype(jnp.float32)
    for block in blocks[1:]:
        total = total + block.astype(jnp.float32)
    return total


def block_terms(row_data, gain_vec, w_gate, w_up, w_down):
    rows32 = row_data.astype(jnp.float32)
    normed = (rows32 * row_scale(rows32) * gain_vec).astype(jnp.bfloat16)
    gate_pre = jnp.dot(normed, w_gate, preferred_element_type=jnp.float32)
    upward = jnp.dot(normed, w_up, preferred_element_type=jnp.float32)
    hidden = (jax.nn.silu(gate_pre) * upward).astype(jnp.bfloat16)
    return jnp.dot(hidden, w_down, preferred_element_type=jnp.float32)


def delta_step(
    query_vec, key_vec, value_vec, gate_vals, beta_gate, head_decay_rate, state, head_norm_gain
):
    both = jnp.stack([key_vec, query_vec], axis=2)
    seen = jnp.einsum("shqd,shde->shqe", both, state, precision=lax.Precision.HIGHEST)
    decay = head_decay_rate[..., None]
    correction = beta_gate[..., None] * (value_vec - decay * seen[:, :, 0])
    new_state = decay[..., None] * state + key_vec[..., :, None] * correction[..., None, :]
    overlap = jnp.sum(key_vec * query_vec, axis=-1, keepdims=True)
    read_out = decay * seen[:, :, 1] + overlap * correction
    normed = read_out * row_scale(read_out) * head_norm_gain
    return (normed * jax.nn.silu(gate_vals), new_state)


def shards(
    tokens,
    first_norm_gain,
    first_gate_weight,
    first_up_weight,
    first_down_weight,
    mixer_norm_gain,
    query_weight,
    key_weight,
    value_weight,
    output_gate_weight,
    strength_weight,
    decay_weight,
    head_decay_log,
    decay_input_bias,
    decay_extra_log,
    head_norm_gain,
    state,
    mixer_output_weight,
    second_norm_gain,
    second_gate_weight,
    second_up_weight,
    second_down_weight,
):
    columns = tokens.shape[1]
    kv_index = lax.axis_index("kv")
    tp_index = lax.axis_index("tp")
    n_kv, n_tp = lax.axis_size("kv"), lax.axis_size("tp")
    seq_dev, heads_dev, head_size = (state.shape[0], state.shape[1], state.shape[2])
    kv_width = query_weight.shape[0]
    head_cols = heads_dev * head_size
    model_width = mixer_norm_gain.shape[0]
    own_rows = kv_index * seq_dev
    head_start = tp_index * heads_dev

    def own_columns(terms):
        blocks = [
            [
                terms[:, (j * n_tp + t) * columns : (j * n_tp + t + 1) * columns]
                for j in range(n_kv)
            ]
            for t in range(n_tp)
        ]
        halves = by_distance([jnp.concatenate(part, axis=1) for part in blocks], tp_index)
        chip_sum = add_up(exchange([half.astype(jnp.bfloat16) for half in halves], "tp"))
        chip_sum = chip_sum.astype(jnp.bfloat16)
        parts = [chip_sum[:, j * columns : (j + 1) * columns] for j in range(n_kv)]
        return add_up(exchange(by_distance(parts, kv_index), "kv"))

    own_parts = jnp.concatenate(gathered(tokens, "kv", kv_index), axis=1)
    tp_parts = gathered(own_parts, "tp", tp_index)
    rows_all = jnp.concatenate(
        [
            tp_parts[t][:, j * columns : (j + 1) * columns]
            for j in range(n_kv)
            for t in range(n_tp)
        ],
        axis=1,
    )
    ffn_terms = block_terms(
        rows_all, first_norm_gain, first_gate_weight, first_up_weight, first_down_weight
    )
    share_sum = own_columns(ffn_terms)
    first_rows = (tokens.astype(jnp.float32) + 0.5 * share_sum).astype(jnp.bfloat16)
    kv_block = jnp.concatenate(gathered(first_rows, "tp", tp_index), axis=1)
    block32 = kv_block.astype(jnp.float32)
    block_gain = lax.dynamic_slice_in_dim(mixer_norm_gain, kv_index * kv_width, kv_width)
    block_scaled = (block32 * block_gain).astype(jnp.bfloat16)
    gate_rows = [
        lax.dynamic_slice(weight, (kv_index * kv_width, head_start), (kv_width, heads_dev))
        for weight in (strength_weight, decay_weight)
    ]
    small = jnp.concatenate(
        [jnp.dot(block_scaled, w, preferred_element_type=jnp.float32) for w in gate_rows]
        + [jnp.sum(block32 * block32, axis=1, keepdims=True)],
        axis=1,
    )
    small = jnp.pad(small, ((0, 0), (0, head_size // 2 - small.shape[1])))
    upper = lax.reduce_precision(small, 8, 7)
    sent = jnp.concatenate(
        [
            jnp.dot(block_scaled, weight, preferred_element_type=jnp.float32)
            for weight in (query_weight, key_weight, value_weight, output_gate_weight)
        ]
        + [upper, small - upper],
        axis=1,
    ).astype(jnp.bfloat16)
    row_parts = [sent[j * seq_dev : (j + 1) * seq_dev] for j in range(n_kv)]
    projected = add_up(exchange(by_distance(row_parts, kv_index), "kv"))
    own_small = (
        projected[:, 4 * head_cols : 4 * head_cols + head_size // 2]
        + projected[:, 4 * head_cols + head_size // 2 :]
    )
    squares = own_small[:, 2 * heads_dev : 2 * heads_dev + 1]
    own_factor = lax.rsqrt(squares / model_width + EPS)

    def split_heads(role_index):
        return (
            projected[:, role_index * head_cols : (role_index + 1) * head_cols] * own_factor
        ).reshape(seq_dev, heads_dev, head_size)

    query_vec = unit_rows(jax.nn.silu(split_heads(0))) * head_size ** (-0.5)
    key_vec = unit_rows(jax.nn.silu(split_heads(1)))
    value_vec = jax.nn.silu(split_heads(2))
    gate_vals = split_heads(3)
    beta_gate = jax.nn.sigmoid(own_small[:, :heads_dev] * own_factor)
    decay_log_term = lax.dynamic_slice_in_dim(head_decay_log, head_start, heads_dev)
    decay_offset_term = lax.dynamic_slice_in_dim(decay_input_bias, head_start, heads_dev)
    head_decay_rate = jnp.exp(
        decay_extra_log
        - jnp.exp(decay_log_term)
        * jax.nn.softplus(
            own_small[:, heads_dev : 2 * heads_dev] * own_factor + decay_offset_term
        )
    )
    heads_f32, new_state = delta_step(
        query_vec, key_vec, value_vec, gate_vals, beta_gate, head_decay_rate, state, head_norm_gain
    )
    heads_out = heads_f32.reshape(seq_dev, head_cols).astype(jnp.bfloat16)
    mixer_terms = jnp.dot(
        jnp.concatenate(gathered(heads_out, "kv", kv_index), axis=0),
        mixer_output_weight,
        preferred_element_type=jnp.float32,
    ).astype(jnp.bfloat16)
    mixer_sum = add_up(
        [mixer_terms] + [lax.ppermute(mixer_terms, "tp", swaps("tp", s)) for s in range(1, n_tp)]
    )
    second_block = (block32 + mixer_sum).astype(jnp.bfloat16)
    rows_last = jnp.concatenate(gathered(second_block, "kv", kv_index), axis=1)
    last_terms = block_terms(
        rows_last, second_norm_gain, second_gate_weight, second_up_weight, second_down_weight
    )
    last_sum = own_columns(last_terms)
    second_rows = by_distance(
        [second_block[:, t * columns : (t + 1) * columns] for t in range(n_tp)], tp_index
    )[0]
    layer_out = (second_rows.astype(jnp.float32) + 0.5 * last_sum).astype(jnp.bfloat16)
    return (layer_out, new_state)


def solution(mesh):
    placed = (
        P("dp", ("kv", "tp")),
        P(),
        P(None, ("kv", "tp")),
        P(None, ("kv", "tp")),
        P(("kv", "tp"), None),
        P(),
        P("kv", "tp"),
        P("kv", "tp"),
        P("kv", "tp"),
        P("kv", "tp"),
        P(),
        P(),
        P(),
        P(),
        P(("dp", "kv"), "tp"),
        P(),
        P(("dp", "kv"), "tp", None, None),
        P("tp", "kv"),
        P(),
        P(None, ("kv", "tp")),
        P(None, ("kv", "tp")),
        P(("kv", "tp"), None),
    )
    return jax.shard_map(
        shards,
        mesh=mesh,
        in_specs=placed,
        out_specs=(P("dp", ("kv", "tp")), P(("dp", "kv"), "tp", None, None)),
        check_vma=False,
    )
```
